32 devices in a mesh: sp: 8 (over z, y), tp: 4 (over x, core).
Axes of the slice: x: 2, y: 2, z: 4, core: 2. Of those that a mesh axis runs over, the one named last changes fastest.
Arguments:
- d_out: bfloat16 [4096, 2048], P('sp'), may hold values from -6 to 6
- route_expert: int32 [4096, 2], P('sp'), may hold values from 0 to 7, all different within a row; in each aligned block of 512 rows (0 to 511, 512 to 1023, ...) at most 144 rows name the same one
- route_weight: float32 [4096, 2], P('sp'), may hold values from 0.2 to 1
- expert_inputs: bfloat16 [8, 1152, 2048], P('sp'), may hold values from -6 to 6
- w_gate: bfloat16 [8, 2048, 2816], P('sp', None, 'tp'), may hold values from -0.125 to 0.125
- w_up: bfloat16 [8, 2048, 2816], P('sp', None, 'tp'), may hold values from -0.125 to 0.125
- w_down: bfloat16 [8, 2816, 2048], P('sp', 'tp'), may hold values from -0.109375 to 0.109375
- w_out: bfloat16 [2048, 1024], P(None, 'tp'), may hold values from -0.1875 to 0.1875
- queries: bfloat16 [4096, 4, 128], P('sp', 'tp'), may hold values from -6 to 6
- keys: bfloat16 [4096, 4, 128], P('sp', 'tp'), may hold values from -2 to 2
- values: bfloat16 [4096, 4, 256], P('sp', 'tp'), may hold values from -6 to 6
- log_decay: float32 [4096, 4, 128], P('sp', 'tp'), may hold values from -1 to 0
Outputs:
- grad_gate: bfloat16 [8, 2048, 2816], P('sp', None, 'tp')
- grad_up: bfloat16 [8, 2048, 2816], P('sp', None, 'tp')
- grad_down: bfloat16 [8, 2816, 2048], P('sp', 'tp')
- grad_proj: float32 [2048, 1024], P('sp', 'tp')
- grad_queries: bfloat16 [4096, 4, 128], P('sp', 'tp')
- grad_keys: bfloat16 [4096, 4, 128], P('sp', 'tp')
- grad_values: bfloat16 [4096, 4, 256], P('sp', 'tp')
- grad_log_decay: float32 [4096, 4, 128], P('sp', 'tp')
The draws below stay inside these ranges and needn't reach their ends.
Inputs may be any that keep to these rules, and one draw needn't show every extreme that they name: `route_expert`: the two experts of a token differ. Among the rows of one device no expert is named more than 144 times, and in every draw some device names some expert exactly 144 times.
All inputs are finite; a program needn't handle non-finite values.
Results may differ from the reference program's by a relative error of at most 0.02.
Values may be sent and summed in bfloat16 or wider, within the bound.
No kernel may reach another device: no remote copies, remote signals or barrier semaphores. Data moves between devices by JAX's collectives and lax.ppermute only.
A program may use at most 128 MiB of HBM per device.

```python
import math
import jax
import jax.numpy as jnp
import numpy as np
from jax import lax

D = 2048
FF = 2816
MIXER_HEADS = 4
KEY_CHANNELS = 128
DV = 256
BLK = 64
TOK_DEV = 512
SEQUENCE_TOKENS = 4096
EXPERTS = 8
CAP = 144
N_SP = 8
N_TP = 4


def draw_log_decay(key, part):
    every_head_keys = jax.random.split(jax.random.fold_in(key, 11), 7)
    slow_share = 0.5
    gradual_decay_mask = jax.random.bernoulli(every_head_keys[0], slow_share, (MIXER_HEADS, KEY_CHANNELS))
    slow_rate = jnp.exp(jax.random.uniform(every_head_keys[1], (MIXER_HEADS, KEY_CHANNELS), jnp.float32, jnp.log(0.05), jnp.log(0.5))) / SEQUENCE_TOKENS
    fast_rate = jnp.exp(jax.random.uniform(every_head_keys[2], (MIXER_HEADS, KEY_CHANNELS), jnp.float32, jnp.log(0.01), jnp.log(0.033)))
    base_rate = jnp.where(gradual_decay_mask, slow_rate, fast_rate)
    segment_count = SEQUENCE_TOKENS // TOK_DEV
    device_factor = jnp.exp(jax.random.uniform(every_head_keys[3], (segment_count, 1, 1, 1), jnp.float32, jnp.log(0.5), jnp.log(2.0)))
    device_factor = jnp.broadcast_to(device_factor, (segment_count, TOK_DEV, 1, 1)).reshape(SEQUENCE_TOKENS, 1, 1)
    roughness = jax.random.uniform(every_head_keys[4], (SEQUENCE_TOKENS, MIXER_HEADS, KEY_CHANNELS), jnp.float32, 0.5, 1.5)
    spike_position = jax.random.randint(every_head_keys[5], (4,), 0, SEQUENCE_TOKENS)
    spike_token_rows = jnp.any(jnp.arange(SEQUENCE_TOKENS)[:, None] == spike_position[None, :], axis=1)
    spike_penalty = jnp.log(jax.random.uniform(every_head_keys[6], (SEQUENCE_TOKENS, MIXER_HEADS, KEY_CHANNELS), jnp.float32, 0.5, 0.8))
    channel_decay_logs = -base_rate[None] * device_factor * roughness
    channel_decay_logs = channel_decay_logs + jnp.where(spike_token_rows[:, None, None] & gradual_decay_mask[None], spike_penalty, 0.0)
    return channel_decay_logs.astype(jnp.float32)


def with_spikes(drawn, own_key, source, target, shards_of, factor):
    def block_of(position):
        return (jnp.arange(drawn.shape[position]) // (drawn.shape[position] // shards_of)).reshape((-1,) + (1,) * (drawn.ndim - 1 - position))

    near = jax.random.permutation(own_key, shards_of)[block_of(target)]
    far = (block_of(target) + shards_of // 2) % shards_of
    return jnp.where((block_of(source) == near) | (block_of(source) == far), factor * drawn, drawn)


def levels(rng, dims, shards, least, largest):
    loudness = 1.0
    for dim, shards_of in shards:
        steps = jax.random.uniform(jax.random.fold_in(jax.random.fold_in(rng, 6), dim), (shards_of,), jnp.float32, least / len(shards), largest / len(shards))
        loudness = loudness * jnp.repeat(jnp.exp(steps), dims[dim] // shards_of).reshape((-1,) + (1,) * (len(dims) - 1 - dim))
    return loudness


def assign_block(own_key, own, number, rows, amount, top, reach, skew):
    ranking = jax.random.permutation(own_key, amount)
    crowded, ordinary = load_shares(amount, rows * top, reach, skew, True), load_shares(amount, rows * top, reach, skew, False)
    places = jnp.arange(amount)

    def named(sizes, turn):
        used = int((sizes > 0).sum())
        fixed = max(1, used // 4)
        passed = fixed + (places - fixed + turn * (used - fixed)) % max(1, amount - fixed)
        return jnp.zeros((amount,), jnp.int32).at[ranking[jnp.where(places < fixed, places, passed)]].set(jnp.asarray(sizes, jnp.int32))

    sizes = jnp.where(number % 4 == 0, named(crowded, number // 4), named(ordinary, number - number // 4 - 1))
    mixed = jax.random.permutation(jax.random.fold_in(own, 3), amount)
    giver, receiver = mixed[0:amount // 2 * 2:2], mixed[1:amount // 2 * 2:2]
    slack = jnp.minimum(sizes[giver] - 1, reach - sizes[receiver]) // 2
    slack = jnp.where((giver == ranking[0]) | (receiver == ranking[0]) | (sizes[receiver] == 0), 0, jnp.maximum(slack, 0))
    passed = jax.random.randint(jax.random.fold_in(own, 4), (amount // 2,), 0, 1 << 20) % (slack + 1)
    sizes = sizes.at[giver].add(-passed).at[receiver].add(passed)
    members = jnp.searchsorted(jnp.cumsum(sizes), jnp.arange(rows * top), side="right").astype(jnp.int32)
    grid = members.reshape(top, rows).T
    grid = grid[jax.random.permutation(jax.random.fold_in(own, 1), rows)]
    turn = jax.random.randint(jax.random.fold_in(own, 2), (rows, 1), 0, top)
    return jnp.take_along_axis(grid, (jnp.arange(top)[None, :] + turn) % top, axis=1)


def load_shares(amount, total, reach, lean, full):
    weights = [(1 << 20) // math.isqrt(grade ** lean) + 1 for grade in range(1, amount + 1)]
    largest = reach if full else min(reach, max(-(-total // amount), total * weights[0] // sum(weights)))
    least = 1 if total - largest >= amount - 1 else 0
    given, surplus = [largest] + [least] * (amount - 1), total - largest - least * (amount - 1)
    while surplus > 0:
        movable = [i for i in range(1, amount) if given[i] < largest] or [i for i in range(1, amount) if given[i] < reach]
        mass, budget = sum([weights[i] for i in movable]), surplus
        for i in movable:
            extra = min(reach - given[i], max(1, budget * weights[i] // mass), surplus)
            given[i] = given[i] + extra
            surplus = surplus - extra
    return np.array(given)


def gaussian(stream_key, shape, width, limit, shards=(), kind=jnp.bfloat16):
    loudness = levels(stream_key, shape, shards, -0.22, 0.18) if shards else 1.0
    entries = jax.random.normal(stream_key, shape, jnp.float32) * width * loudness
    return jnp.minimum(jnp.maximum(entries, -limit), limit).astype(kind)


def gaussian_with(rng, dims, scale, bound, cuts, heavy, kind=jnp.bfloat16):
    values = scale * jax.random.normal(rng, dims, jnp.float32)
    if cuts:
        values = values * levels(rng, dims, cuts, -0.22, 0.18)
    return jnp.clip(with_spikes(values, jax.random.fold_in(rng, 3), *heavy), -bound, bound).astype(kind)


def setup_inputs(seed: int = 0) -> dict:
    splits = jax.random.split(jax.random.key(seed), 13)
    d_out = gaussian_with(splits[0], (SEQUENCE_TOKENS, D), 1.0, 6.0, ((0, 8),), (0, 1, 8, 2.0))
    route_expert_keys = jax.random.split(jax.random.fold_in(splits[1], 1), SEQUENCE_TOKENS // TOK_DEV)
    route_expert_turns = jax.random.permutation(jax.random.fold_in(splits[1], 3), SEQUENCE_TOKENS // TOK_DEV)
    route_expert = jax.vmap(lambda own, number: assign_block(jax.random.fold_in(splits[1], 2), own, number, TOK_DEV, EXPERTS, 2, CAP, 0))(route_expert_keys, route_expert_turns).reshape((SEQUENCE_TOKENS, 2))
    route_weight = jnp.clip(0.2 + 0.8 * jax.random.uniform(splits[2], (SEQUENCE_TOKENS, 2), jnp.float32) ** levels(splits[2], (SEQUENCE_TOKENS, 2), ((0, 8),), -0.2, 0.2), 0.2, 1.0)
    expert_inputs = gaussian(splits[3], (EXPERTS, EXPERTS * CAP, D), 1.0, 6.0, ((0, 8),))
    w_gate = gaussian(splits[4], (EXPERTS, D, FF), D ** -0.5, 0.125, ((0, 8), (2, 4)))
    w_up = gaussian(splits[5], (EXPERTS, D, FF), D ** -0.5, 0.125, ((0, 8), (2, 4)))
    w_down = gaussian(splits[6], (EXPERTS, FF, D), FF ** -0.5, 0.109375, ((0, 8), (1, 4)))
    w_out = gaussian(splits[7], (D, MIXER_HEADS * DV), (MIXER_HEADS * DV) ** -0.5, 0.1875, ((1, 4),))
    queries = gaussian(splits[8], (SEQUENCE_TOKENS, MIXER_HEADS, KEY_CHANNELS), 1.0, 6.0, ((0, 8), (1, 4)))
    keys = gaussian(splits[9], (SEQUENCE_TOKENS, MIXER_HEADS, KEY_CHANNELS), (SEQUENCE_TOKENS ** -0.25), 2.0, ((0, 8), (1, 4)))
    values = gaussian(splits[10], (SEQUENCE_TOKENS, MIXER_HEADS, DV), 1.0, 6.0, ((0, 8), (1, 4)))
    log_decay = draw_log_decay(jax.random.fold_in(splits[12], 71), 0)
    return dict(d_out=d_out, route_expert=route_expert, route_weight=route_weight, expert_inputs=expert_inputs, w_gate=w_gate, w_up=w_up, w_down=w_down, w_out=w_out, queries=queries, keys=keys, values=values, log_decay=log_decay)


precise = lax.Precision.HIGHEST

def block_mixer(scaled_queries, keys_in, values_in, decay_in, initial):
    length, head_count, _ = scaled_queries.shape
    value_width = values_in.shape[-1]
    count_blocks = length // BLK

    def to_blocks(tensor):
        return tensor.reshape(count_blocks, BLK, head_count, tensor.shape[-1]).transpose(0, 2, 1, 3)
    causal = jnp.tril(jnp.ones((BLK, BLK), dtype=bool))[:, :, None]

    def advance(carry_state, inputs):
        query_block, key_block, value_block, decay_block = inputs
        cumulative = jnp.cumsum(decay_block, axis=1)
        ending = cumulative[:, -1, :]
        carried = jnp.einsum('hcd,hde->hce', query_block * jnp.exp(cumulative), carry_state, precision=precise)
        within = jnp.where(causal, jnp.exp(cumulative[:, :, None, :] - cumulative[:, None, :, :]), 0.0)
        scores = jnp.einsum('hid,hjd,hijd->hij', query_block, key_block, within, precision=precise)
        inner_part = jnp.einsum('hij,hje->hie', scores, value_block, precision=precise)
        faded_keys = key_block * jnp.exp(ending[:, None, :] - cumulative)
        carry_state = carry_state * jnp.exp(ending)[:, :, None] + jnp.einsum('hcd,hce->hde', faded_keys, value_block, precision=precise)
        return (carry_state, carried + inner_part)
    final_state, blocks_out = lax.scan(jax.checkpoint(advance), initial, (to_blocks(scaled_queries), to_blocks(keys_in), to_blocks(values_in), to_blocks(decay_in)))
    return (blocks_out.transpose(0, 2, 1, 3).reshape(length, head_count, value_width), final_state)

def expert_pass(rows_in, routed_rows, gate_w, up_w, down_w):
    gate_pre = jnp.dot(rows_in, gate_w, preferred_element_type=jnp.float32)
    up_pre = jnp.dot(rows_in, up_w, preferred_element_type=jnp.float32)
    sigmoid_gate = jax.nn.sigmoid(gate_pre)
    active = gate_pre * sigmoid_gate
    hidden = (active * up_pre).astype(jnp.bfloat16)
    d_hidden = lax.dot_general(routed_rows, down_w, (((1,), (1,)), ((), ())), preferred_element_type=jnp.float32)
    d_gate = (d_hidden * up_pre * sigmoid_gate * (1.0 + gate_pre * (1.0 - sigmoid_gate))).astype(jnp.bfloat16)
    d_up = (d_hidden * active).astype(jnp.bfloat16)
    rows_first = (((0,), (0,)), ((), ()))
    grad_gate = lax.dot_general(rows_in, d_gate, rows_first, preferred_element_type=jnp.float32).astype(jnp.bfloat16)
    grad_up = lax.dot_general(rows_in, d_up, rows_first, preferred_element_type=jnp.float32).astype(jnp.bfloat16)
    grad_down = lax.dot_general(hidden, routed_rows, rows_first, preferred_element_type=jnp.float32).astype(jnp.bfloat16)
    return (grad_gate, grad_up, grad_down, d_gate, d_up)

def reference(d_out, route_expert, route_weight, expert_inputs, w_gate, w_up, w_down, w_out, queries, keys, values, log_decay):
    per_block = route_expert.reshape(N_SP, 2 * TOK_DEV).astype(jnp.int32)
    onehot = (per_block[:, :, None] == jnp.arange(EXPERTS, dtype=jnp.int32)[None, None, :]).astype(jnp.int32)
    before = jnp.cumsum(onehot, axis=1) - onehot
    rank_slot = lax.optimization_barrier(jnp.sum(before * onehot, axis=2))
    source_dev = jnp.arange(N_SP, dtype=jnp.int32)[:, None]
    slot_index = (per_block * (N_SP * CAP) + source_dev * CAP + rank_slot).reshape(-1).astype(jnp.int32)
    scaled = (jnp.repeat(d_out, 2, axis=0).astype(jnp.float32) * route_weight.reshape(-1)[:, None]).astype(jnp.bfloat16)
    routed = jnp.zeros((EXPERTS * N_SP * CAP, D), jnp.bfloat16).at[slot_index].set(scaled).reshape(EXPERTS, N_SP * CAP, D)
    part_width = FF // N_TP

    def one_expert(operands):
        rows_in, routed_rows, gate_w, up_w, down_w = operands
        grad_gate, grad_up, grad_down, d_gate, d_up = expert_pass(rows_in, routed_rows, gate_w, up_w, down_w)
        total = jnp.zeros((rows_in.shape[0], D), jnp.float32)
        for piece in range(N_TP):
            lower = piece * part_width
            term = lax.dot_general(d_gate[:, lower:lower + part_width], gate_w[:, lower:lower + part_width], (((1,), (1,)), ((), ())), preferred_element_type=jnp.float32)
            term = term + lax.dot_general(d_up[:, lower:lower + part_width], up_w[:, lower:lower + part_width], (((1,), (1,)), ((), ())), preferred_element_type=jnp.float32)
            total = total + lax.optimization_barrier(term.astype(jnp.bfloat16)).astype(jnp.float32)
        return (grad_gate, grad_up, grad_down, total.astype(jnp.bfloat16))
    grad_gate, grad_up, grad_down, row_grads = lax.map(one_expert, (expert_inputs, routed, w_gate, w_up, w_down))
    picked = row_grads.reshape(-1, D)[slot_index].astype(jnp.float32).reshape(SEQUENCE_TOKENS, 2, D).sum(axis=1)
    mix_grad = (d_out.astype(jnp.float32) + picked).astype(jnp.bfloat16)
    scale_q = KEY_CHANNELS ** (-0.5)
    initial = jnp.zeros((MIXER_HEADS, KEY_CHANNELS, DV), jnp.float32)

    def mixer_map(query_x, key_x, value_x, decay_x):
        return block_mixer(query_x * scale_q, key_x, value_x, decay_x, initial)[0]
    mixer_out, pullback = jax.vjp(mixer_map, queries.astype(jnp.float32), keys.astype(jnp.float32), values.astype(jnp.float32), log_decay)
    mixed = mixer_out.reshape(SEQUENCE_TOKENS, MIXER_HEADS * DV).astype(jnp.bfloat16)
    grad_proj = lax.dot_general(mix_grad, mixed, (((0,), (0,)), ((), ())), preferred_element_type=jnp.float32)
    d_mixed = jnp.dot(mix_grad, w_out, preferred_element_type=jnp.float32).reshape(SEQUENCE_TOKENS, MIXER_HEADS, DV)
    grad_q, grad_k, grad_v, grad_g = pullback(d_mixed)
    return (grad_gate, grad_up, grad_down, grad_proj, grad_q.astype(jnp.bfloat16), grad_k.astype(jnp.bfloat16), grad_v.astype(jnp.bfloat16), grad_g)
```

```python
import functools

import jax
import jax.numpy as jnp
from jax import lax
from jax.experimental import pallas as pl
from jax.experimental.pallas import tpu as pltpu
from jax.sharding import PartitionSpec as P


BLK = 64
CARRY_PAD = 16
VMEM_BYTES = 14 * 1024 * 1024
F32 = jnp.float32
BF16 = jnp.bfloat16
EXACT = lax.Precision.HIGHEST


def whole(shape):
    return pl.BlockSpec(shape, lambda _: (0,) * len(shape))


def call(kernel, outs, args, flops, scalar=None):
    moved = sum(a.size * a.dtype.itemsize for a in args)
    moved += sum(o.size * o.dtype.itemsize for o in jax.tree.leaves(outs))
    first = () if scalar is None else (scalar,)
    return pl.pallas_call(
        kernel,
        grid=(1,),
        out_shape=outs,
        in_specs=[pl.BlockSpec(memory_space=pltpu.SMEM)] * len(first)
        + [whole(a.shape) for a in args],
        out_specs=jax.tree.map(lambda o: whole(o.shape), outs),
        compiler_params=pltpu.CompilerParams(vmem_limit_bytes=VMEM_BYTES),
        cost_estimate=pl.CostEstimate(flops=flops, bytes_accessed=moved, transcendentals=0),
    )(*first, *args)


def dot_nn(a, b, precision=None):
    return lax.dot_general(
        a, b, (((1,), (0,)), ((), ())), preferred_element_type=F32, precision=precision
    )


def dot_nt(a, b):
    return lax.dot_general(a, b, (((1,), (1,)), ((), ())), preferred_element_type=F32)


def dot_tn(a, b):
    return lax.dot_general(a, b, (((0,), (0,)), ((), ())), preferred_element_type=F32)


def triangle(size, compare):
    rows = lax.broadcasted_iota(jnp.int32, (size, size), 0)
    cols = lax.broadcasted_iota(jnp.int32, (size, size), 1)
    return compare(rows, cols)


def dispatch_kernel(cuts, experts, pos_ref, ids_t_ref, gain_t_ref, rows_ref, *refs):
    *boxes, own_ref, slots_ref, sem = refs
    width = own_ref.shape[1]
    column = pl.multiple_of(pos_ref[0] * width, width)
    fetch = pltpu.make_async_copy(rows_ref.at[:, pl.ds(column, width)], own_ref, sem)
    fetch.start()
    tokens = ids_t_ref.shape[1]
    ids_t = ids_t_ref[...]
    names = lax.broadcasted_iota(jnp.int32, (experts, tokens), 0)
    first_t = (names == ids_t[0:1, :]).astype(F32)
    second_t = (names == ids_t[1:2, :]).astype(F32)
    earlier = triangle(tokens, lambda r, c: r < c).astype(BF16)
    before_t = dot_nn((first_t + second_t).astype(BF16), earlier)
    rank_a = jnp.sum(before_t * first_t, axis=0, keepdims=True).astype(jnp.int32)
    rank_b = jnp.sum(before_t * second_t, axis=0, keepdims=True).astype(jnp.int32)
    both = [ids_t.astype(F32), gain_t_ref[...], jnp.zeros((4, tokens), F32)]
    columns = jnp.concatenate(both, axis=0).T
    ids, gain = columns[:, 0:2].astype(jnp.int32), columns[:, 2:4]
    labels = lax.broadcasted_iota(jnp.int32, (tokens, experts), 1)
    first = (labels == ids[:, 0:1]).astype(F32)
    second = (labels == ids[:, 1:2]).astype(F32)
    later = triangle(tokens, lambda r, c: r > c).astype(BF16)
    before = dot_nn(later, (first + second).astype(BF16))
    col_a = jnp.sum(before * first, axis=1, keepdims=True).astype(jnp.int32)
    col_b = jnp.sum(before * second, axis=1, keepdims=True).astype(jnp.int32)
    slots_ref[:, 0:1] = slot_of(cuts, experts, ids[:, 0:1], col_a)
    slots_ref[:, 1:2] = slot_of(cuts, experts, ids[:, 1:2], col_b)
    slot_a = slot_of(cuts, experts, ids_t[0:1, :], rank_a)
    slot_b = slot_of(cuts, experts, ids_t[1:2, :], rank_b)
    fetch.wait()
    own = own_ref[...].astype(F32)
    scaled_a = (own * gain[:, 0:1]).astype(BF16)
    scaled_b = (own * gain[:, 1:2]).astype(BF16)
    start = 0
    for box in boxes:
        count = box.shape[0]
        here = lax.broadcasted_iota(jnp.int32, (count, tokens), 0) + start
        pick_a = jnp.where(here == slot_a, 1.0, 0.0).astype(BF16)
        pick_b = jnp.where(here == slot_b, 1.0, 0.0).astype(BF16)
        box[...] = (dot_nn(pick_a, scaled_a) + dot_nn(pick_b, scaled_b)).astype(BF16)
        start += count


def slot_of(cuts, experts, expert, rank):
    slot = expert * cuts[0][1] + rank
    for low, size in cuts[1:]:
        slot = jnp.where(rank >= low, experts * low + expert * size + (rank - low), slot)
    return slot


def dispatch(cuts, experts, position, route_expert, route_weight, d_out, width):
    tokens = d_out.shape[0]
    rows = experts * sum(size for _, size in cuts)
    outs = [jax.ShapeDtypeStruct((experts * size, width), BF16) for _, size in cuts]
    outs.append(jax.ShapeDtypeStruct((tokens, width), BF16))
    outs.append(jax.ShapeDtypeStruct((tokens, 2), jnp.int32))
    everything = lambda *_: (0, 0)
    return pl.pallas_call(
        functools.partial(dispatch_kernel, cuts, experts),
        grid_spec=pltpu.PrefetchScalarGridSpec(
            num_scalar_prefetch=1,
            grid=(1,),
            in_specs=[
                pl.BlockSpec((2, tokens), everything),
                pl.BlockSpec((2, tokens), everything),
                pl.BlockSpec(memory_space=pltpu.HBM),
            ],
            out_specs=[pl.BlockSpec(o.shape, everything) for o in outs],
            scratch_shapes=[pltpu.SemaphoreType.DMA],
        ),
        out_shape=outs,
        compiler_params=pltpu.CompilerParams(vmem_limit_bytes=VMEM_BYTES),
        cost_estimate=pl.CostEstimate(
            flops=4 * rows * tokens * width, bytes_accessed=1 << 21, transcendentals=0
        ),
        name="dispatch",
    )(position, route_expert.T, route_weight.T, d_out)


def collect_kernel(slots_ref, rows_ref, *refs):
    boxes, out_ref = refs[:-1], refs[-1]
    slots = slots_ref[...]
    tokens = slots.shape[0]
    total = rows_ref[...].astype(F32)
    start = 0
    for box in boxes:
        count = box.shape[0]
        here = lax.broadcasted_iota(jnp.int32, (tokens, count), 1) + start
        hit = (here == slots[:, 0:1]) | (here == slots[:, 1:2])
        total = total + dot_nn(jnp.where(hit, 1.0, 0.0).astype(BF16), box[...])
        start += count
    out_ref[...] = total.astype(BF16)


def block_sums(g_ref):
    upto = triangle(BLK, lambda r, c: r >= c).astype(F32)
    sums, ends = [], []
    for n in range(g_ref.shape[0] // BLK):
        c = dot_nn(upto, g_ref[n * BLK : (n + 1) * BLK, :], EXACT)
        sums.append(c)
        ends.append(c[BLK - 1 : BLK, :])
    return sums, ends


def store_carry(pay_ref, state, decay):
    rows = state.shape[0]
    pay_ref[0:rows, :] = state.astype(BF16)
    pay_ref[rows:, :] = jnp.broadcast_to(decay, (pay_ref.shape[0] - rows, decay.shape[1])).astype(
        BF16
    )


def produced_kernel(k_ref, v_ref, g_ref, pay_ref):
    sums, ends = block_sums(g_ref)
    after = jnp.zeros_like(ends[0])
    faded = [None] * len(sums)
    for n in reversed(range(len(sums))):
        after = after + ends[n]
        k = k_ref[n * BLK : (n + 1) * BLK, :].astype(F32)
        faded[n] = (k * jnp.exp(after - sums[n])).astype(BF16)
    store_carry(pay_ref, dot_tn(v_ref[...], jnp.concatenate(faded, 0)), jnp.exp(after))


def forward_kernel(scale, odd_ref, q_ref, k_ref, v_ref, g_ref, other_ref, *refs):
    part_refs, (mixed_ref, states_ref) = refs[:-2], refs[-2:]
    sums, ends = block_sums(g_ref)
    causal = triangle(BLK, lambda r, c: r >= c)
    state = entering(False, odd_ref, other_ref, part_refs)
    for n, (c, end) in enumerate(zip(sums, ends)):
        at = slice(n * BLK, (n + 1) * BLK)
        k = k_ref[at, :].astype(F32)
        v = v_ref[at, :]
        grown = (q_ref[at, :].astype(F32) * (scale * jnp.exp(c))).astype(BF16)
        shrunk = (k * jnp.exp(-c)).astype(BF16)
        faded = (k * jnp.exp(end - c)).astype(BF16)
        now = state.astype(BF16)
        states_ref[n] = now
        scores = jnp.where(causal, dot_nt(grown, shrunk), 0.0).astype(BF16)
        mixed_ref[at, :] = (dot_nt(grown, now) + dot_nn(scores, v)).astype(BF16)
        state = state * jnp.exp(end) + dot_tn(v, faded)


def cotangent_kernel(scale, d_ref, q_ref, g_ref, pay_ref):
    sums, ends = block_sums(g_ref)
    upto = jnp.zeros_like(ends[0])
    grown = []
    for n, c in enumerate(sums):
        q = q_ref[n * BLK : (n + 1) * BLK, :].astype(F32)
        grown.append((q * (scale * jnp.exp(upto + c))).astype(BF16))
        upto = upto + ends[n]
    store_carry(pay_ref, dot_tn(d_ref[...], jnp.concatenate(grown, 0)), jnp.exp(upto))


def backward_kernel(scale, odd_ref, q_ref, k_ref, v_ref, g_ref, states_ref, d_ref, other_ref, *refs):
    part_refs, (dq_ref, dk_ref, dv_ref, dg_ref) = refs[:-4], refs[-4:]
    sums, ends = block_sums(g_ref)
    causal = triangle(BLK, lambda r, c: r >= c)
    onward = triangle(BLK, lambda r, c: r <= c).astype(F32)
    earlier = triangle(BLK, lambda r, c: r > c).astype(F32)
    d_state = entering(True, odd_ref, other_ref, part_refs)
    for n in reversed(range(len(sums))):
        at = slice(n * BLK, (n + 1) * BLK)
        c, end = sums[n], ends[n]
        k = k_ref[at, :].astype(F32)
        v = v_ref[at, :]
        d_out = d_ref[at, :]
        state = states_ref[n]
        up, down, fade, whole = jnp.exp(c), jnp.exp(-c), jnp.exp(end - c), jnp.exp(end)
        grown = (q_ref[at, :].astype(F32) * (scale * up)).astype(BF16)
        shrunk = (k * down).astype(BF16)
        faded = (k * fade).astype(BF16)
        d_now = d_state.astype(BF16)
        scores = jnp.where(causal, dot_nt(grown, shrunk), 0.0).astype(BF16)
        d_scores = jnp.where(causal, dot_nt(d_out, v), 0.0).astype(BF16)
        dv_ref[at, :] = (dot_tn(scores, d_out) + dot_nt(faded, d_now)).astype(BF16)
        d_grown = dot_nn(d_out, state) + dot_nn(d_scores, shrunk)
        d_shrunk = dot_tn(d_scores, grown)
        d_faded = dot_nn(v, d_now)
        dq_ref[at, :] = (d_grown * (scale * up)).astype(BF16)
        dk_ref[at, :] = (d_shrunk * down + d_faded * fade).astype(BF16)
        inner = grown.astype(F32) * d_grown - shrunk.astype(F32) * d_shrunk
        outer = faded.astype(F32) * d_faded
        kept = jnp.sum(d_now.astype(F32) * state.astype(F32), axis=0, keepdims=True) * whole
        dg_ref[at, :] = dot_nn(onward, inner, EXACT) + dot_nn(earlier, outer, EXACT) + kept
        d_state = d_state * whole + dot_tn(d_out, grown)


def split_carry(ref):
    rows = ref.shape[0] - CARRY_PAD
    return ref[0:rows, :].astype(F32), ref[rows : rows + 1, :].astype(F32)


def pair_kernel(reverse, odd_ref, mine_ref, other_ref, pay_ref):
    leads = (odd_ref[0] == 1) if reverse else (odd_ref[0] == 0)
    mine, mine_decay = split_carry(mine_ref)
    other, other_decay = split_carry(other_ref)
    state = jnp.where(leads, mine * other_decay + other, other * mine_decay + mine)
    store_carry(pay_ref, state, mine_decay * other_decay)


def entering(reverse, odd_ref, other_ref, part_refs):
    other, decay = split_carry(other_ref)
    state = jnp.zeros_like(other)
    for ref in reversed(part_refs):
        own, own_decay = split_carry(ref)
        state = state * own_decay + own
    follows = (odd_ref[0] == 0) if reverse else (odd_ref[0] == 1)
    return jnp.where(follows, state * decay + other, state)


def exchange_carry(pay, odd, reverse):
    count = lax.axis_size("sp")
    if count % 2:
        raise ValueError("mesh sizes")
    step = -2 if reverse else 2
    other = lax.ppermute(pay, "sp", [(s, s ^ 1) for s in range(count)])
    pair = call(
        functools.partial(pair_kernel, reverse),
        jax.ShapeDtypeStruct(pay.shape, pay.dtype),
        (pay, other),
        1 << 28,
        odd,
    )
    parts = []
    for away in range(1, count // 2):
        pairs = [(s, s + step * away) for s in range(count) if 0 <= s + step * away < count]
        parts.append(lax.ppermute(pair, "sp", pairs))
    return [other] + parts


def tp_swap(x, mask):
    count = lax.axis_size("tp")
    return lax.ppermute(x, "tp", [(s, s ^ mask) for s in range(count)])


def gather_tp(x):
    held = {0: x}
    mask = lax.axis_size("tp") >> 1
    while mask:
        held.update({at ^ mask: tp_swap(part, mask) for at, part in list(held.items())})
        mask >>= 1
    return [held[d] for d in sorted(held)]


def scatter_tp(pieces):
    mask = 1
    while len(pieces) > 1:
        pieces = {
            d: (pieces[d].astype(F32) + tp_swap(pieces[d ^ mask], mask).astype(F32)).astype(BF16)
            for d in sorted(pieces)
            if not d & mask
        }
        mask <<= 1
    return pieces[0]


def sp_to_all(x):
    return lax.all_to_all(x, "sp", split_axis=0, concat_axis=0, tiled=True)


def scatter_proj(x, bands):
    count, index, width = lax.axis_size("sp"), lax.axis_index("sp"), lax.axis_size("tp")
    masks = [1 << n for n in range(count.bit_length() - 1)]
    for stage, mask in enumerate(masks):
        axis = 0 if (1 << stage) < bands else 1
        bit = (index // mask) % 2
        half = x.shape[axis] // 2
        keep = lax.dynamic_slice_in_dim(x, bit * half, half, axis)
        send = lax.dynamic_slice_in_dim(x, (1 - bit) * half, half, axis)
        if mask == masks[-1]:
            break
        got = lax.ppermute(send, "sp", [(s, s ^ mask) for s in range(count)])
        x = (keep.astype(F32) + got.astype(F32)).astype(BF16)

    def home(s, t):
        block = 0
        for mask in masks:
            block = block * 2 + (s // mask) % 2
        band, part = divmod(block, width)
        return (t * bands + band) * width + (t ^ part)

    devices = [(s, t) for s in range(count) for t in range(width)]
    first = lax.ppermute(
        send, ("sp", "tp"), [(s * width + t, home(s ^ masks[-1], t)) for s, t in devices]
    )
    second = lax.ppermute(
        keep, ("sp", "tp"), [(s * width + t, home(s, t)) for s, t in devices]
    )
    return first.astype(F32) + second.astype(F32)


def local(
    d_out,
    route_expert,
    route_weight,
    expert_inputs,
    w_gate,
    w_up,
    w_down,
    w_out,
    queries,
    keys,
    values,
    log_decay,
):
    tokens, model_width = d_out.shape
    experts, tp_count = lax.axis_size("sp"), lax.axis_size("tp")
    capacity = expert_inputs.shape[1] // experts
    quarter = model_width // tp_count
    tp_index = lax.axis_index("tp")
    position = tp_index.astype(jnp.int32).reshape(1)
    odd = (lax.axis_index("sp") & 1).astype(jnp.int32).reshape(1)
    half = capacity // 2
    if half % 8:
        half = capacity
    cuts = [(0, half)] + ([(half, capacity - half)] if half < capacity else [])

    if tp_count & (tp_count - 1) or experts & (experts - 1) or experts % tp_count:
        raise ValueError("mesh sizes")
    others = range(tp_count)

    *boxes, own_cols, slots = dispatch(
        cuts, experts, position, route_expert, route_weight, d_out, quarter
    )
    arrived = [
        sp_to_all(box.reshape(experts, size, quarter)).reshape(experts * size, quarter)
        for box, (_, size) in zip(boxes, cuts)
    ]
    routed = [gather_tp(part) for part in arrived]

    w_rows = [
        lax.dynamic_slice_in_dim(w_out, (tp_index ^ d) * quarter, quarter, 0) for d in others
    ]
    w_rows = [w_rows[0]] + [tp_swap(w_rows[d], d) for d in others if d]
    reversed_bits = [0]
    while len(reversed_bits) < tp_count:
        reversed_bits = [2 * r for r in reversed_bits] + [2 * r + 1 for r in reversed_bits]
    w_rows = jnp.concatenate([w_rows[d] for d in reversed_bits], 1)

    heads = queries.shape[1]
    scale = queries.shape[2] ** (-0.5)
    dk, dv = queries.shape[2], values.shape[2]
    blocks = tokens // BLK
    pay_shape = jax.ShapeDtypeStruct((dv + CARRY_PAD, dk), BF16)
    per_head = []
    for h in range(heads):
        q, k, v, g = queries[:, h], keys[:, h], values[:, h], log_decay[:, h]
        k, v, g, slots = lax.optimization_barrier((k, v, g, slots))
        pay = call(produced_kernel, pay_shape, (k, v, g), 1 << 30)
        carries = exchange_carry(pay, odd, False)
        mixed, states = call(
            functools.partial(forward_kernel, scale),
            (
                jax.ShapeDtypeStruct((tokens, dv), BF16),
                jax.ShapeDtypeStruct((blocks, dv, dk), BF16),
            ),
            (q, k, v, g, *carries),
            1 << 31,
            odd,
        )
        per_head.append((q, k, v, g, mixed, states))
    mixed = jnp.concatenate([p[4] for p in per_head], 1) if heads > 1 else per_head[0][4]

    by_rank = expert_inputs[0].reshape(experts, capacity, model_width)
    rows_in = [
        by_rank[:, low : low + size].reshape(experts * size, model_width) for low, size in cuts
    ]
    gate_w, up_w, down_w = w_gate[0], w_up[0], w_down[0]
    spot = [(tp_index ^ d) * quarter for d in others]
    gates, ups, hiddens, returned = [], [], [], []
    for rows, pieces, (_, size) in zip(rows_in, routed, cuts):
        gate_pre = jnp.dot(rows, gate_w, preferred_element_type=F32)
        up_pre = jnp.dot(rows, up_w, preferred_element_type=F32)
        sigmoid_gate = jax.nn.sigmoid(gate_pre)
        active = gate_pre * sigmoid_gate
        hiddens.append((active * up_pre).astype(BF16))
        d_hidden = None
        for d in sorted(others, key=lambda d: d & 1):
            term = dot_nt(pieces[d], lax.dynamic_slice_in_dim(down_w, spot[d], quarter, 1))
            d_hidden = term if d_hidden is None else d_hidden + term
        d_gate = (
            d_hidden * up_pre * sigmoid_gate * (1.0 + gate_pre * (1.0 - sigmoid_gate))
        ).astype(BF16)
        d_up = (d_hidden * active).astype(BF16)
        gates.append(d_gate)
        ups.append(d_up)
        terms = {}
        for d in reversed(others):
            term = dot_nt(d_gate, lax.dynamic_slice_in_dim(gate_w, spot[d], quarter, 0))
            term = term + dot_nt(d_up, lax.dynamic_slice_in_dim(up_w, spot[d], quarter, 0))
            terms[d] = term.astype(BF16)
        summed = scatter_tp(terms)
        returned.append(
            sp_to_all(summed.reshape(experts, size, quarter)).reshape(experts * size, quarter)
        )
    mixed_all = jnp.concatenate(gather_tp(mixed), 1)
    all_rows = jnp.concatenate(rows_in, 0)
    grad_gate = dot_tn(all_rows, jnp.concatenate(gates, 0)).astype(BF16)
    grad_up = dot_tn(all_rows, jnp.concatenate(ups, 0)).astype(BF16)
    all_hidden = jnp.concatenate(hiddens, 0)
    grad_down = jnp.zeros((down_w.shape[0], model_width), BF16)
    for d in others:
        column = jnp.concatenate([pieces[d] for pieces in routed], 0)
        grad_down = lax.dynamic_update_slice_in_dim(
            grad_down, dot_tn(all_hidden, column).astype(BF16), spot[d], 1
        )
    slots, grad_up, grad_down, mixed_all, w_rows = lax.optimization_barrier(
        (slots, grad_up, grad_down, mixed_all, w_rows)
    )
    mix_cols = call(
        collect_kernel,
        jax.ShapeDtypeStruct(own_cols.shape, BF16),
        (slots, own_cols, *returned),
        1 << 30,
    )

    mask, held = 1, None
    while mask < tp_count:
        half_cols = (w_rows if held is None else held).shape[1] // 2
        if held is None:
            send = jnp.dot(mix_cols, w_rows[:, half_cols:], preferred_element_type=F32).astype(BF16)
            keep = jnp.dot(mix_cols, w_rows[:, :half_cols], preferred_element_type=F32)
        else:
            send, keep = held[:, half_cols:], held[:, :half_cols].astype(F32)
        held = (keep + tp_swap(send, mask).astype(F32)).astype(BF16)
        mask <<= 1
    d_mixed_all = held
    grad_proj = scatter_proj(dot_tn(mix_cols, mixed_all).astype(BF16), experts // tp_count)
    grads = []
    for h, (q, k, v, g, _, states) in enumerate(per_head):
        d_mixed = d_mixed_all[:, h * dv : (h + 1) * dv]
        pay = call(functools.partial(cotangent_kernel, scale), pay_shape, (d_mixed, q, g), 1 << 30)
        carries = exchange_carry(pay, odd, True)
        grads.append(
            call(
                functools.partial(backward_kernel, scale),
                (
                    jax.ShapeDtypeStruct((tokens, dk), BF16),
                    jax.ShapeDtypeStruct((tokens, dk), BF16),
                    jax.ShapeDtypeStruct((tokens, dv), BF16),
                    jax.ShapeDtypeStruct((tokens, dk), F32),
                ),
                (q, k, v, g, states, d_mixed, *carries),
                1 << 32,
                odd,
            )
        )
    grad_q, grad_k, grad_v, grad_g = (jnp.stack(parts, 1) for parts in zip(*grads))
    return (
        grad_gate[None],
        grad_up[None],
        grad_down[None],
        grad_proj,
        grad_q,
        grad_k,
        grad_v,
        grad_g,
    )


def solution(mesh):
    return mapped(mesh)


def mapped(mesh):
    return jax.shard_map(
        local,
        mesh=mesh,
        in_specs=(
            P("sp", None),
            P("sp", None),
            P("sp", None),
            P("sp", None, None),
            P("sp", None, "tp"),
            P("sp", None, "tp"),
            P("sp", "tp", None),
            P(None, "tp"),
            P("sp", "tp", None),
            P("sp", "tp", None),
            P("sp", "tp", None),
            P("sp", "tp", None),
        ),
        out_specs=(
            P("sp", None, "tp"),
            P("sp", None, "tp"),
            P("sp", "tp", None),
            P("sp", "tp"),
            P("sp", "tp", None),
            P("sp", "tp", None),
            P("sp", "tp", None),
            P("sp", "tp", None),
        ),
        check_vma=False,
    )
```
